128 devices in a mesh: sp: 64 (over z, y, x), tp: 2 (over core).
Axes of the slice: x: 4, y: 4, z: 4, core: 2. Of those that a mesh axis runs over, the one named last changes fastest.
Arguments:
- query_rows: bfloat16 [16384, 1024], P('sp', 'tp'), may hold values from -26 to 26
- key_rows: bfloat16 [16384, 128], P('sp', 'tp'), may hold values from -26 to 26
- value_head_rows: bfloat16 [16384, 128], P('sp', 'tp'), may hold values from -6 to 6
- sink_logit_head: float32 [16], P('tp'), may hold values from -6 to 6
- out_weight: bfloat16 [1024, 2048], P('tp'), may hold values from -0.1875 to 0.1875
- residual: bfloat16 [16384, 2048], P(('sp', 'tp')), may hold values from -6 to 6
- norm_gain: float32 [2048], replicated, may hold values from 0.1 to 1.9
- routes: int32 [16384, 2], P(('sp', 'tp')), may hold values from 0 to 63, all different within a row; in each aligned block of 128 rows (0 to 127, 128 to 255, ...) at most 6 rows name the same one
- route_weights: float32 [16384, 2], P(('sp', 'tp')), may hold values from 0.1 to 1
- gate_proj: bfloat16 [64, 2048, 3584], P('sp', None, 'tp'), may hold values from -0.125 to 0.125
- up_proj: bfloat16 [64, 2048, 3584], P('sp', None, 'tp'), may hold values from -0.125 to 0.125
- down_proj: bfloat16 [64, 3584, 2048], P('sp', 'tp'), may hold values from -0.09375 to 0.09375
Outputs:
- output: bfloat16 [16384, 2048], P(('sp', 'tp'))
The draws below stay inside these ranges and needn't reach their ends.
Inputs may be any that keep to these rules, and one draw needn't show every extreme that they name: `routes`: A row names 2 different experts. Among the rows of one device no expert is named more than 6 times, a bound that some block reaches on some devices.
All inputs are finite; a program needn't handle non-finite values.
Results may differ from the reference program's by a relative error of at most 0.0055.
Values may be sent and summed in bfloat16 or wider, within the bound.
A program may use at most 128 MiB of HBM per device.

```python
import math
import jax
import jax.numpy as jnp
import numpy as np
from jax import lax

D = 2048
QUERY_HEADS = 16
KEY_VALUE_HEADS = 2
HEAD_SIZE = 64
FF = 3584
TOP = 2
WINDOW_KEYS = 128
TOKENS_PER_SHARD = 256
SEQUENCE_TOKENS = 16384
ROWS_DEV = 128
EXPERTS = 64
CAP = 6
N_SP = 64
N_TP = 2


def draw_query_rows(key, part):
    start_offset = jnp.clip(jax.random.normal(jax.random.fold_in(key, 1), (SEQUENCE_TOKENS, QUERY_HEADS * HEAD_SIZE), jnp.float32), -6.0, 6.0)
    return start_offset.astype(jnp.bfloat16)


def draw_key_rows(key, part):
    start_offset = jnp.clip(jax.random.normal(jax.random.fold_in(key, 2), (SEQUENCE_TOKENS, KEY_VALUE_HEADS * HEAD_SIZE), jnp.float32), -6.0, 6.0)
    return start_offset.astype(jnp.bfloat16)


def shard_levels(stream_key, extent, pieces, least, top_value):
    gain, own = 1.0, jax.random.fold_in(stream_key, 6)
    for dim, parts in pieces:
        draws = jnp.exp(jax.random.uniform(jax.random.fold_in(own, dim), (parts,), jnp.float32, least / len(pieces), top_value / len(pieces)))
        gain = gain * jnp.repeat(draws, extent[dim] // parts).reshape([-1 if axis == dim else 1 for axis in range(len(extent))])
    return gain


def routed_block(key, own, number, rows, count, top, reach, lean):
    ranking = jax.random.permutation(key, count)
    heavy_load, ordinary = load_shares(count, rows * top, reach, lean, True), load_shares(count, rows * top, reach, lean, False)
    places = jnp.arange(count)

    def named(tallies, offset_by):
        used = int((tallies > 0).sum())
        fixed = max(1, used // 4)
        shifted = fixed + (places - fixed + offset_by * (used - fixed)) % max(1, count - fixed)
        return jnp.zeros((count,), jnp.int32).at[ranking[jnp.where(places < fixed, places, shifted)]].set(jnp.asarray(tallies, jnp.int32))

    tallies = jnp.where(number % 4 == 0, named(heavy_load, number // 4), named(ordinary, number - number // 4 - 1))
    mixed = jax.random.permutation(jax.random.fold_in(own, 3), count)
    giver, receiver = mixed[0:count // 2 * 2:2], mixed[1:count // 2 * 2:2]
    slack = jnp.minimum(tallies[giver] - 1, reach - tallies[receiver]) // 2
    slack = jnp.where((giver == ranking[0]) | (receiver == ranking[0]) | (tallies[receiver] == 0), 0, jnp.maximum(slack, 0))
    shifted = jax.random.randint(jax.random.fold_in(own, 4), (count // 2,), 0, 1 << 20) % (slack + 1)
    tallies = tallies.at[giver].add(-shifted).at[receiver].add(shifted)
    items = jnp.searchsorted(jnp.cumsum(tallies), jnp.arange(rows * top), side="right").astype(jnp.int32)
    table = items.reshape(top, rows).T
    table = table[jax.random.permutation(jax.random.fold_in(own, 1), rows)]
    offset_by = jax.random.randint(jax.random.fold_in(own, 2), (rows, 1), 0, top)
    return jnp.take_along_axis(table, (jnp.arange(top)[None, :] + offset_by) % top, axis=1)


def load_shares(count, total, limit, lean, full):
    loads = [(1 << 20) // math.isqrt(standing ** lean) + 1 for standing in range(1, count + 1)]
    largest = limit if full else min(limit, max(-(-total // count), total * loads[0] // sum(loads)))
    least = 1 if total - largest >= count - 1 else 0
    holding, surplus = [largest] + [least] * (count - 1), total - largest - least * (count - 1)
    while surplus > 0:
        candidates = [i for i in range(1, count) if holding[i] < largest] or [i for i in range(1, count) if holding[i] < limit]
        mass, remaining = sum([loads[i] for i in candidates]), surplus
        for i in candidates:
            addition = min(limit - holding[i], max(1, remaining * loads[i] // mass), surplus)
            holding[i] = holding[i] + addition
            surplus = surplus - addition
    return np.array(holding)


def normal_values(rng, dims, spread, limit, shards=(), kind=jnp.bfloat16):
    array = jax.random.normal(rng, dims, jnp.float32) * spread
    if len(shards) > 0:
        array = shard_levels(rng, dims, shards, -0.22, 0.18) * array
    return jnp.clip(array, min=-limit, max=limit).astype(kind)


def setup_inputs(seed: int = 0) -> dict:
    key_list = jax.random.split(jax.random.key(seed), 13)
    query_rows = draw_query_rows(jax.random.fold_in(key_list[12], 71), 0)
    key_rows = draw_key_rows(jax.random.fold_in(key_list[12], 71), 0)
    value_head_rows = normal_values(key_list[2], (SEQUENCE_TOKENS, KEY_VALUE_HEADS * HEAD_SIZE), 1.0, 6.0, ((0, 64), (1, 2)))
    sink_logit_head = normal_values(key_list[3], (QUERY_HEADS,), 2.0, 6.0, ((0, 2),), jnp.float32)
    out_weight = normal_values(key_list[4], (QUERY_HEADS * HEAD_SIZE, D), (QUERY_HEADS * HEAD_SIZE) ** -0.5, 0.1875, ((0, 2),))
    residual = normal_values(key_list[5], (SEQUENCE_TOKENS, D), 1.0, 6.0, ((0, 128),))
    norm_gain = jnp.clip(1.0 + 0.18 * jax.random.normal(key_list[6], (D,), jnp.float32), 0.1, 1.9)
    routes_keys = jax.random.split(jax.random.fold_in(key_list[7], 1), SEQUENCE_TOKENS // ROWS_DEV)
    routes_turns = jax.random.permutation(jax.random.fold_in(key_list[7], 3), SEQUENCE_TOKENS // ROWS_DEV)
    routes = jax.vmap(lambda own, number: routed_block(jax.random.fold_in(key_list[7], 2), own, number, ROWS_DEV, EXPERTS, TOP, CAP, 2))(routes_keys, routes_turns).reshape((SEQUENCE_TOKENS, TOP))
    route_weights = jnp.clip(0.1 + 0.9 * jax.random.uniform(key_list[8], (SEQUENCE_TOKENS, TOP), jnp.float32) ** shard_levels(key_list[8], (SEQUENCE_TOKENS, TOP), ((0, 128),), -0.2, 0.2), 0.1, 1.0)
    gate_proj = normal_values(key_list[9], (EXPERTS, D, FF), D ** -0.5, 0.125, ((0, 64), (2, 2)))
    up_proj = normal_values(key_list[10], (EXPERTS, D, FF), D ** -0.5, 0.125, ((0, 64), (2, 2)))
    down_proj = normal_values(key_list[11], (EXPERTS, FF, D), FF ** -0.5, 0.09375, ((0, 64), (1, 2)))
    return {"query_rows": query_rows, "key_rows": key_rows, "value_head_rows": value_head_rows, "sink_logit_head": sink_logit_head, "out_weight": out_weight, "residual": residual, "norm_gain": norm_gain, "routes": routes, "route_weights": route_weights, "gate_proj": gate_proj, "up_proj": up_proj, "down_proj": down_proj}


def attention_all(query_rows, key_rows, value_head_rows, sink_logit_head):
    query_group = QUERY_HEADS // KEY_VALUE_HEADS
    blocks = SEQUENCE_TOKENS // TOKENS_PER_SHARD
    leading_edge = jnp.zeros((WINDOW_KEYS, KEY_VALUE_HEADS * HEAD_SIZE), jnp.bfloat16)
    key_pad = jnp.concatenate([leading_edge, key_rows], axis=0)
    value_pad = jnp.concatenate([leading_edge, value_head_rows], axis=0)
    slope_values = jnp.exp2(-8.0 * jnp.arange(1, QUERY_HEADS + 1, dtype=jnp.float32) / QUERY_HEADS).reshape(KEY_VALUE_HEADS, query_group)
    sink_portion = sink_logit_head.astype(jnp.float32).reshape(KEY_VALUE_HEADS, query_group)[:, :, None]

    def attend(block):
        start = (block * TOKENS_PER_SHARD).astype(jnp.int32)
        query_vector = lax.dynamic_slice_in_dim(query_rows, start, TOKENS_PER_SHARD, 0).astype(jnp.float32)
        key_block = lax.dynamic_slice_in_dim(key_pad, start, TOKENS_PER_SHARD + WINDOW_KEYS, 0).astype(jnp.float32)
        value_block = lax.dynamic_slice_in_dim(value_pad, start, TOKENS_PER_SHARD + WINDOW_KEYS, 0).astype(jnp.float32)
        score_matrix = jnp.einsum('rjwh,cjh->jwrc', query_vector.reshape(TOKENS_PER_SHARD, KEY_VALUE_HEADS, query_group, HEAD_SIZE), key_block.reshape(-1, KEY_VALUE_HEADS, HEAD_SIZE)) * HEAD_SIZE ** (-0.5)
        query_pos = start + jnp.arange(TOKENS_PER_SHARD, dtype=jnp.int32)
        key_pos = start - WINDOW_KEYS + jnp.arange(TOKENS_PER_SHARD + WINDOW_KEYS, dtype=jnp.int32)
        distance = query_pos[:, None] - key_pos[None, :]
        inside = (distance >= 0) & (distance < WINDOW_KEYS) & (key_pos[None, :] >= 0)
        score_matrix = score_matrix - slope_values[:, :, None, None] * distance.astype(jnp.float32)[None, None]
        score_matrix = jnp.where(inside[None, None], score_matrix, -jnp.inf)
        peak = jnp.maximum(lax.optimization_barrier(jnp.max(score_matrix, axis=-1)), sink_portion)
        expd = jnp.exp(score_matrix - peak[..., None])
        denom = lax.optimization_barrier(jnp.sum(expd, axis=-1)) + jnp.exp(sink_portion - peak)
        probabilities = (expd / denom[..., None]).astype(jnp.bfloat16)
        final_output = jnp.einsum('wfbt,twj->bwfj', probabilities.astype(jnp.float32), value_block.reshape(-1, KEY_VALUE_HEADS, HEAD_SIZE))
        return final_output.reshape(TOKENS_PER_SHARD, QUERY_HEADS * HEAD_SIZE).astype(jnp.bfloat16)
    outs = lax.map(attend, jnp.arange(blocks, dtype=jnp.int32))
    return outs.reshape(SEQUENCE_TOKENS, QUERY_HEADS * HEAD_SIZE)

def reference(query_rows, key_rows, value_head_rows, sink_logit_head, out_weight, residual, norm_gain, routes, route_weights, gate_proj, up_proj, down_proj):
    attended = attention_all(query_rows, key_rows, value_head_rows, sink_logit_head)
    mixed = residual.astype(jnp.float32) + jnp.dot(attended, out_weight, preferred_element_type=jnp.float32)
    scale = lax.rsqrt(lax.optimization_barrier(jnp.mean(mixed * mixed, axis=-1, keepdims=True)) + 1e-05)
    normed = (mixed * scale * norm_gain).astype(jnp.bfloat16)
    devices = N_SP * N_TP
    per_dev = ROWS_DEV * TOP
    chosen = routes.reshape(devices, per_dev).astype(jnp.int32)
    onehot = (chosen[:, :, None] == jnp.arange(EXPERTS, dtype=jnp.int32)[None, None, :]).astype(jnp.int32)
    running = jnp.cumsum(onehot, axis=1).astype(jnp.int32)
    rank_in = (lax.optimization_barrier(jnp.sum(onehot * running, axis=-1)) - 1).astype(jnp.int32)
    source = jnp.arange(devices, dtype=jnp.int32)[:, None]
    slot_index = ((chosen * devices + source) * CAP + rank_in).astype(jnp.int32)
    token_of = (source * ROWS_DEV + jnp.arange(per_dev, dtype=jnp.int32)[None, :] // TOP).astype(jnp.int32)
    slots_all = EXPERTS * devices * CAP
    table = jnp.full((slots_all,), SEQUENCE_TOKENS, jnp.int32).at[slot_index.reshape(-1)].set(token_of.reshape(-1))
    normed_pad = jnp.concatenate([normed, jnp.zeros((1, D), jnp.bfloat16)], axis=0)
    half = FF // 2

    def expert(index):
        picks = lax.dynamic_slice_in_dim(table, (index * devices * CAP).astype(jnp.int32), devices * CAP, 0)
        rows_in = normed_pad[picks]
        gate = jnp.dot(rows_in, gate_proj[index], preferred_element_type=jnp.float32)
        upper = jnp.dot(rows_in, up_proj[index], preferred_element_type=jnp.float32)
        hidden = (jax.nn.silu(gate) * upper).astype(jnp.bfloat16)
        down = down_proj[index]
        first = jnp.dot(hidden[:, :half], down[:half], preferred_element_type=jnp.float32).astype(jnp.bfloat16)
        second = jnp.dot(hidden[:, half:], down[half:], preferred_element_type=jnp.float32).astype(jnp.bfloat16)
        first, second = lax.optimization_barrier((first, second))
        return (first.astype(jnp.float32) + second.astype(jnp.float32)).astype(jnp.bfloat16)
    results = lax.map(expert, jnp.arange(EXPERTS, dtype=jnp.int32)).reshape(slots_all, D)
    picked = results[slot_index.reshape(-1)].reshape(SEQUENCE_TOKENS, TOP, D)
    moe_sum = lax.optimization_barrier(jnp.sum(route_weights[:, :, None] * picked.astype(jnp.float32), axis=1))
    return (mixed + moe_sum).astype(jnp.bfloat16)
```

```python
import functools

import jax
import jax.numpy as jnp
from jax import lax
from jax.experimental import pallas as pl
from jax.experimental.pallas import tpu as pltpu
from jax.sharding import PartitionSpec as P

QUERY_HEADS = 16
KEY_VALUE_HEADS = 2
HEAD_SIZE = 64
TOP = 2
WINDOW_KEYS = 128

MESH = pl.DeviceIdType.MESH
F32 = jnp.float32
BF16 = jnp.bfloat16

ROWS = 128
D = 2048
FFH = 1792
CAP = 6
Q = 4
W = D // Q
BLK = Q * CAP
CH = 4
PER = 16
GB = 8
GR = GB * CAP


def from_behind(block, axis, distance):
    devices = range(lax.axis_size(axis))
    route = [(i - distance, i) for i in devices if i - distance in devices]
    return lax.ppermute(block, axis, route)


def in_blocks(shard, dim, size):
    before, after = (shard.shape[:dim], shard.shape[dim + 1 :])
    return jnp.moveaxis(shard.reshape(*before, size, -1, *after), dim, 0)


def summed_on_arrival(shard, axis, dim):
    size = lax.axis_size(axis)
    tiles = lax.all_to_all(in_blocks(shard, dim, size), axis, 0, 0, tiled=True)
    return jnp.sum(tiles, axis=0)


def fiota(shape, dim):
    return lax.broadcasted_iota(jnp.int32, shape, dim).astype(F32)


def fdiv(v, n):
    return jnp.floor((v + 0.5) * (1.0 / n))


def offset_of(g, i):
    dz = i % 4
    dy = (i // 4 + i) % 4
    dx = (g + 8 - dz - dy) % 4
    return dx, dy, dz


def block_facts(g, r, x, y, z):
    i = fdiv(r, BLK)
    rest = r - i * BLK
    q = fdiv(rest, CAP)
    s = rest - q * CAP
    hi = fdiv(i, 4)
    dz = i - hi * 4
    dy = (hi + dz) - 4.0 * fdiv(hi + dz, 4)
    dx = (g + 8 - dz - dy) - 4.0 * fdiv(g + 8 - dz - dy, 4)
    ex = (x + dx) - 4.0 * fdiv(x + dx, 4)
    ey = (y + dy) - 4.0 * fdiv(y + dy, 4)
    ez = (z + dz) - 4.0 * fdiv(z + dz, 4)
    return ez * 16 + ey * 4 + ex, q, s


def moe_kernel(
    mixed_ref,
    gain_ref,
    routes_ref,
    rw_ref,
    wg_hbm,
    wu_hbm,
    wd_hbm,
    out_ref,
    wg,
    wu,
    wd,
    nrm,
    sbuf,
    mine,
    other,
    xbuf,
    hid,
    pm,
    po,
    pr,
    ysend,
    zbuf,
    acc,
    wsem,
    dsend,
    drecv,
    fsend,
    frecv,
    psend,
    precv,
    rsend,
    rrecv,
):
    sp = lax.axis_index("sp")
    tp = lax.axis_index("tp")
    x, y, z = sp % 4, (sp // 4) % 4, sp // 16
    partner = (sp, 1 - tp)

    wcopies = []
    for k, (src, dst) in enumerate(((wg_hbm, wg), (wu_hbm, wu), (wd_hbm, wd))):
        part = src.shape[1] // 4
        for j in range(4):
            rows = pl.ds(j * part, part)
            wcopies.append(pltpu.make_async_copy(src.at[0, rows], dst.at[rows], wsem.at[k, j]))
    for c in wcopies:
        c.start()

    barrier = pltpu.get_barrier_semaphore()

    def greet(i, _):
        pl.semaphore_signal(barrier, inc=1, device_id=((sp + i) % 64, tp), device_id_type=MESH)
        return 0

    lax.fori_loop(1, 64, greet, 0)
    pl.semaphore_signal(barrier, inc=1, device_id=partner, device_id_type=MESH)

    m = mixed_ref[...]
    scale = lax.rsqrt(jnp.mean(m * m, axis=-1, keepdims=True) + 1e-05)
    n = (m * scale * gain_ref[...]).astype(BF16)
    for q in range(Q):
        nrm[q * ROWS : (q + 1) * ROWS, :] = n[:, q * W : (q + 1) * W]
        acc[q * ROWS : (q + 1) * ROWS, :] = m[:, q * W : (q + 1) * W]

    xf, yf, zf = x.astype(F32), y.astype(F32), z.astype(F32)
    routes = routes_ref[...].astype(F32)
    r0c = jnp.broadcast_to(routes[:, 0:1], (ROWS, ROWS))
    r1c = jnp.broadcast_to(routes[:, 1:2], (ROWS, ROWS))
    ri, ci = fiota((ROWS, ROWS), 0), fiota((ROWS, ROWS), 1)
    eye = jnp.where(ri == ci, 1.0, 0.0)
    r0 = jnp.sum(r0c * eye, axis=0, keepdims=True)
    r1 = jnp.sum(r1c * eye, axis=0, keepdims=True)
    upper = jnp.where(ri < ci, 1.0, 0.0).astype(BF16)
    lower = jnp.where(ci < ri, 1.0, 0.0).astype(BF16)

    def build(g):
        e, q, s = block_facts(g, fiota((PER * BLK, ROWS), 0), xf, yf, zf)
        cnt = jnp.where((e == r0) | (e == r1), 1.0, 0.0)
        rank = jnp.dot(cnt.astype(BF16), upper, preferred_element_type=F32)
        sel = jnp.where(rank == s, cnt, 0.0)
        parts = [jnp.where(q == k, sel, 0.0).astype(BF16) for k in range(Q)]
        onehot = jnp.concatenate(parts, axis=1)
        rows = jnp.dot(onehot, nrm[...], preferred_element_type=F32).astype(BF16)
        rows = rows.reshape(PER, BLK, W)
        sbuf[pl.ds(g * PER, PER)] = rows
        if g == 0:
            mine[0] = rows[0]

    def lo_of(g):
        return 1 if g == 0 else 0

    def exchange(g, src, dst, ssem, rsem, sign):
        def one(i, _):
            dx, dy, dz = offset_of(g, i)
            peer = (
                ((z + sign * dz + 4) % 4) * 16
                + ((y + sign * dy + 4) % 4) * 4
                + (x + sign * dx + 4) % 4
            )
            pltpu.make_async_remote_copy(
                src_ref=src.at[g * PER + i],
                dst_ref=dst.at[g * PER + i],
                send_sem=ssem.at[g],
                recv_sem=rsem.at[g],
                device_id=(peer, tp),
                device_id_type=MESH,
            ).start()
            return 0

        lax.fori_loop(lo_of(g), PER, one, 0)

    def whole(g, src, dst, ssem, rsem):
        rows = pl.ds(g * PER + lo_of(g), PER - lo_of(g))
        return pltpu.make_async_remote_copy(
            src_ref=src.at[rows],
            dst_ref=dst.at[rows],
            send_sem=ssem.at[g],
            recv_sem=rsem.at[g],
            device_id=partner,
            device_id_type=MESH,
        )

    def forward(g):
        rows = pl.ds(g * PER, PER)
        return pltpu.make_async_remote_copy(
            src_ref=mine.at[rows],
            dst_ref=other.at[rows],
            send_sem=fsend.at[g],
            recv_sem=frecv.at[g],
            device_id=partner,
            device_id_type=MESH,
        )

    def swap(g):
        return pltpu.make_async_remote_copy(
            src_ref=po.at[g],
            dst_ref=pr.at[g],
            send_sem=psend.at[g],
            recv_sem=precv.at[g],
            device_id=partner,
            device_id_type=MESH,
        )

    build(0)
    pl.semaphore_wait(barrier, 64)
    exchange(0, sbuf, mine, dsend, drecv, 1)
    for g in range(1, CH):
        build(g)
        exchange(g, sbuf, mine, dsend, drecv, 1)

    pi, pj = fiota((GB * BLK, GB * BLK), 0), fiota((GB * BLK, GB * BLK), 1)
    iq = fdiv(pi, GR)
    ib = fdiv(pi - iq * GR, CAP)
    ist = pi - iq * GR - ib * CAP
    unpack = jnp.where(ib * BLK + iq * CAP + ist == pj, 1.0, 0.0).astype(BF16)
    jq = fdiv(pj, GR)
    jb = fdiv(pj - jq * GR, CAP)
    js = pj - jq * GR - jb * CAP
    pack = jnp.where(jb * BLK + jq * CAP + js == pi, 1.0, 0.0).astype(BF16)

    def spread(g):
        for h in range(4):
            src = mine if h < 2 else other
            blocks = src[pl.ds(g * PER + (h % 2) * GB, GB)].reshape(GB * BLK, W)
            rows = jnp.dot(unpack, blocks, preferred_element_type=F32).astype(BF16)
            for q in range(Q):
                xbuf[h * GR : (h + 1) * GR, q * W : (q + 1) * W] = rows[q * GR : (q + 1) * GR]

    def gate_up():
        def tile(k, _):
            cols = pl.ds(pl.multiple_of(k * 256, 256), 256)
            a = jnp.dot(xbuf[...], wg[:, cols], preferred_element_type=F32)
            b = jnp.dot(xbuf[...], wu[:, cols], preferred_element_type=F32)
            hid[:, cols] = (a / (1.0 + jnp.exp(-a)) * b).astype(BF16)
            return 0

        lax.fori_loop(0, FFH // 256, tile, 0)

    def down(g):
        def tile(k, _):
            cols = pl.ds(pl.multiple_of(k * 512, 512), 512)
            a = jnp.dot(hid[...], wd[:, cols], preferred_element_type=F32).astype(BF16)
            pm[:, cols] = a[: 2 * GR]
            po[g, :, cols] = a[2 * GR :]
            return 0

        lax.fori_loop(0, D // 512, tile, 0)

    def give_back(g):
        swap(g).wait_recv()
        for h in range(2):
            rows = slice(h * GR, (h + 1) * GR)
            total = (pm[rows].astype(F32) + pr[g, rows].astype(F32)).astype(BF16)
            stack = jnp.concatenate([total[:, q * W : (q + 1) * W] for q in range(Q)], axis=0)
            packed = jnp.dot(pack, stack, preferred_element_type=F32).astype(BF16)
            packed = packed.reshape(GB, BLK, W)
            ysend[pl.ds(g * PER + h * GB, GB)] = packed
            if g == 0 and h == 0:
                zbuf[0] = packed[0]
        exchange(g, ysend, zbuf, rsend, rrecv, -1)

    whole(0, sbuf, mine, dsend, drecv).wait_recv()
    forward(0).start()
    for c in wcopies:
        c.wait()
    for g in range(CH):
        forward(g).wait_recv()
        spread(g)
        if g > 0:
            give_back(g - 1)
        gate_up()
        if g + 1 < CH:
            whole(g + 1, sbuf, mine, dsend, drecv).wait_recv()
            forward(g + 1).start()
        down(g)
        swap(g).start()
    give_back(CH - 1)

    w0, w1 = rw_ref[:, 0:1], rw_ref[:, 1:2]
    c0, c1 = routes[:, 0:1], routes[:, 1:2]
    for g in range(CH):
        e, q, s = block_facts(g, fiota((ROWS, PER * BLK), 1), xf, yf, zf)
        is0, is1 = e == c0, e == c1
        cnt = jnp.where(is0 | is1, 1.0, 0.0)
        rank = jnp.dot(lower, cnt.astype(BF16), preferred_element_type=F32)
        wt = jnp.where(is0, w0, 0.0) + jnp.where(is1, w1, 0.0)
        wt = jnp.where(rank == s, wt, 0.0)
        whi = wt.astype(BF16)
        wlo = (wt - whi.astype(F32)).astype(BF16)
        whole(g, ysend, zbuf, rsend, rrecv).wait_recv()
        back = zbuf[pl.ds(g * PER, PER)].reshape(PER * BLK, W)
        for k in range(Q):
            here = q == k
            hi = jnp.where(here, whi.astype(F32), 0.0).astype(BF16)
            lo = jnp.where(here, wlo.astype(F32), 0.0).astype(BF16)
            both = jnp.dot(hi, back, preferred_element_type=F32) + jnp.dot(
                lo, back, preferred_element_type=F32
            )
            rows = slice(k * ROWS, (k + 1) * ROWS)
            if g + 1 < CH:
                acc[rows] += both
            else:
                out_ref[:, k * W : (k + 1) * W] = (acc[rows] + both).astype(BF16)

    for g in range(CH):
        whole(g, sbuf, mine, dsend, drecv).wait_send()
        forward(g).wait_send()
        swap(g).wait_send()
        whole(g, ysend, zbuf, rsend, rrecv).wait_send()


def moe(mixed, gain, routes, route_weights, gate_proj, up_proj, down_proj):
    vm = pl.BlockSpec(memory_space=pltpu.VMEM)
    hbm = pl.BlockSpec(memory_space=pl.ANY)
    sem = pltpu.SemaphoreType.DMA
    return pl.pallas_call(
        moe_kernel,
        out_shape=jax.ShapeDtypeStruct((ROWS, D), BF16),
        in_specs=[vm, vm, vm, vm, hbm, hbm, hbm],
        out_specs=vm,
        scratch_shapes=[
            pltpu.VMEM((D, FFH), BF16),
            pltpu.VMEM((D, FFH), BF16),
            pltpu.VMEM((FFH, D), BF16),
            pltpu.VMEM((Q * ROWS, W), BF16),
            pltpu.VMEM((CH * PER, BLK, W), BF16),
            pltpu.VMEM((CH * PER, BLK, W), BF16),
            pltpu.VMEM((CH * PER, BLK, W), BF16),
            pltpu.VMEM((4 * GR, D), BF16),
            pltpu.VMEM((4 * GR, FFH), BF16),
            pltpu.VMEM((2 * GR, D), BF16),
            pltpu.VMEM((CH, 2 * GR, D), BF16),
            pltpu.VMEM((CH, 2 * GR, D), BF16),
            pltpu.VMEM((CH * PER, BLK, W), BF16),
            pltpu.VMEM((CH * PER, BLK, W), BF16),
            pltpu.VMEM((Q * ROWS, W), F32),
            sem((3, 4)),
            sem((CH,)),
            sem((CH,)),
            sem((CH,)),
            sem((CH,)),
            sem((CH,)),
            sem((CH,)),
            sem((CH,)),
            sem((CH,)),
        ],
        compiler_params=pltpu.CompilerParams(
            collective_id=0, has_side_effects=True, vmem_limit_bytes=60 * 1024 * 1024
        ),
        name="moe",
    )(mixed, gain.reshape(1, D), routes, route_weights, gate_proj, up_proj, down_proj)


def on_device(
    query_rows,
    key_rows,
    value_head_rows,
    sink_logit_head,
    out_weight,
    residual,
    norm_gain,
    routes,
    route_weights,
    gate_proj,
    up_proj,
    down_proj,
):
    length = query_rows.shape[0]
    query_group = QUERY_HEADS // KEY_VALUE_HEADS
    width = key_rows.shape[1]
    local_kv = width // HEAD_SIZE
    local_heads = local_kv * query_group
    sp_index = lax.axis_index("sp")
    tp_index = lax.axis_index("tp")
    tail = jnp.concatenate(
        [key_rows[length - WINDOW_KEYS :], value_head_rows[length - WINDOW_KEYS :]], axis=1
    )
    before = from_behind(tail, "sp", 1)
    key_all = jnp.concatenate([before[:, :width], key_rows], axis=0)
    value_all = jnp.concatenate([before[:, width:], value_head_rows], axis=0)
    score_matrix = jnp.einsum(
        "rjwh,cjh->jwrc",
        query_rows.reshape(length, local_kv, query_group, HEAD_SIZE),
        key_all.reshape(-1, local_kv, HEAD_SIZE),
        preferred_element_type=jnp.float32,
    ) * HEAD_SIZE ** (-0.5)
    query_pos = sp_index * length + jnp.arange(length, dtype=jnp.int32)
    key_pos = sp_index * length - WINDOW_KEYS + jnp.arange(length + WINDOW_KEYS, dtype=jnp.int32)
    distance = query_pos[:, None] - key_pos[None, :]
    inside = (distance >= 0) & (distance < WINDOW_KEYS) & (key_pos[None, :] >= 0)
    head_ids = (tp_index * local_heads + jnp.arange(local_heads, dtype=jnp.int32)).astype(
        jnp.float32
    )
    slope_values = jnp.exp2(-8.0 * (head_ids + 1.0) / QUERY_HEADS).reshape(local_kv, query_group)
    score_matrix = (
        score_matrix - slope_values[:, :, None, None] * distance.astype(jnp.float32)[None, None]
    )
    score_matrix = jnp.where(inside[None, None], score_matrix, -jnp.inf)
    sink_portion = sink_logit_head.reshape(local_kv, query_group)[:, :, None]
    peak = jnp.maximum(jnp.max(score_matrix, axis=-1), sink_portion)
    expd = jnp.exp(score_matrix - peak[..., None])
    denom = jnp.sum(expd, axis=-1) + jnp.exp(sink_portion - peak)
    probabilities = (expd / denom[..., None]).astype(jnp.bfloat16)
    attended = (
        jnp.einsum(
            "wfbt,twj->bwfj",
            probabilities,
            value_all.reshape(-1, local_kv, HEAD_SIZE),
            preferred_element_type=jnp.float32,
        )
        .reshape(length, local_heads * HEAD_SIZE)
        .astype(jnp.bfloat16)
    )
    projected = summed_on_arrival(
        jnp.dot(attended, out_weight, preferred_element_type=jnp.float32), "tp", 0
    )
    mixed = residual.astype(jnp.float32) + projected
    return moe(mixed, norm_gain, routes, route_weights, gate_proj, up_proj, down_proj)


def solution(mesh):
    placed = (
        P("sp", "tp"),
        P("sp", "tp"),
        P("sp", "tp"),
        P("tp"),
        P("tp", None),
        P(("sp", "tp"), None),
        P(),
        P(("sp", "tp"), None),
        P(("sp", "tp"), None),
        P("sp", None, "tp"),
        P("sp", None, "tp"),
        P("sp", "tp", None),
    )
    return jax.shard_map(
        on_device, mesh=mesh, in_specs=placed, out_specs=P(("sp", "tp"), None), check_vma=False
    )
```

```python
import jax
import jax.numpy as jnp
from jax import lax
from jax.experimental import pallas as pl
from jax.experimental.pallas import tpu as pltpu
from jax.sharding import PartitionSpec as P

MESH = pl.DeviceIdType.MESH
F32 = jnp.float32
BF16 = jnp.bfloat16

HEADS = 8
HEAD_SIZE = 64
KEYS = 128
ROWS = 128
D = 2048
FFH = 1792
CAP = 6
Q = 4
W = D // Q
BLK = Q * CAP
CH = 4
PER = 16
GB = 8
GR = GB * CAP


def offset_chunks():
    def hops(o):
        return sum(min(v, 4 - v) for v in o)

    def opposite(o):
        return tuple((4 - v) % 4 for v in o)

    every = [(a, b, c) for a in range(4) for b in range(4) for c in range(4)]
    by = {h: [o for o in every if hops(o) == h] for h in range(7)}
    axial = [o for o in by[2] if 2 in o]
    same = [o for o in by[2] if 2 not in o and len(set(v for v in o if v)) == 1]
    mixed = [o for o in by[2] if 2 not in o and o not in same]
    corners = [o for o in by[3] if 2 not in o]
    sides = [o for o in by[3] if 2 in o]
    first = by[0] + by[1] + axial + same
    last = corners + sides[:1] + [opposite(sides[0])] + mixed
    rest = [o for o in by[6] + by[5] + by[4] + by[3] if o not in last]
    middle = [[], []]
    done = set()
    for o in rest:
        if o in done:
            continue
        pair = [o] if opposite(o) == o else [o, opposite(o)]
        done.update(pair)
        middle[0 if len(middle[0]) <= len(middle[1]) else 1] += pair
    while len(middle[0]) > PER:
        middle[1].append(middle[0].pop())
    while len(middle[1]) > PER:
        middle[0].append(middle[1].pop())
    return [first, middle[0], middle[1], last]


CHUNKS = offset_chunks()


def fiota(shape, dim):
    return lax.broadcasted_iota(jnp.int32, shape, dim).astype(F32)


def fdiv(v, n):
    return jnp.floor((v + 0.5) * (1.0 / n))


def layer_kernel(
    q_ref,
    kt_ref,
    vt_ref,
    sink_ref,
    gain_ref,
    routes_ref,
    rw_ref,
    wo_hbm,
    res_hbm,
    wg_hbm,
    wu_hbm,
    wd_hbm,
    out_ref,
    wo,
    res,
    wg,
    wu,
    wd,
    halo,
    kk,
    vv,
    att,
    pj,
    pjr,
    nrm,
    onehot,
    comb_hi,
    comb_lo,
    sbuf,
    mine,
    other,
    xbuf,
    hid,
    pm,
    po,
    pr,
    ysend,
    zbuf,
    acc,
    osem,
    wsem,
    hsend,
    hrecv,
    jsend,
    jrecv,
    dsend,
    drecv,
    fsend,
    frecv,
    psend,
    precv,
    rsend,
    rrecv,
):
    sp = lax.axis_index("sp")
    tp = lax.axis_index("tp")
    x, y, z = sp % 4, (sp // 4) % 4, sp // 16
    partner = (sp, 1 - tp)

    barrier = pltpu.get_barrier_semaphore()

    def greet(i, _):
        pl.semaphore_signal(barrier, inc=1, device_id=((sp + i) % 64, tp), device_id_type=MESH)
        return 0

    lax.fori_loop(1, 64, greet, 0)
    pl.semaphore_signal(barrier, inc=1, device_id=partner, device_id_type=MESH)

    ocopies = [
        pltpu.make_async_copy(wo_hbm, wo, osem.at[0]),
        pltpu.make_async_copy(res_hbm, res, osem.at[1]),
    ]
    for c in ocopies:
        c.start()
    wcopies = []
    for k, (src, dst) in enumerate(((wg_hbm, wg), (wu_hbm, wu), (wd_hbm, wd))):
        part = src.shape[1] // 4
        for j in range(4):
            rows = pl.ds(j * part, part)
            wcopies.append(pltpu.make_async_copy(src.at[0, rows], dst.at[rows], wsem.at[k, j]))

    qi, kc = fiota((KEYS, 2 * KEYS), 0), fiota((KEYS, 2 * KEYS), 1)
    dist = qi + KEYS - kc
    window = (dist >= 0.0) & (dist < KEYS)
    tier = jnp.where(tp == 0, 1.0, 2.0 ** (-HEADS / 2)).astype(F32)
    first = jnp.where(sp == 0, float(KEYS), 0.0).astype(F32)
    kk[...] = jnp.zeros_like(kk)
    vv[...] = jnp.zeros_like(vv)

    def attend(b):
        for ref, own, n in ((kk, kt_ref, 0), (vv, vt_ref, 1)):
            for h in range(2):
                rows = slice(h * HEAD_SIZE, (h + 1) * HEAD_SIZE)
                lane = h * 2 * KEYS
                if b == 1:
                    ref[rows, lane : lane + 2 * KEYS] = own[...]
                else:
                    ref[rows, lane : lane + KEYS] = halo[n]
                    ref[rows, lane + KEYS : lane + 2 * KEYS] = own[:, :KEYS]
        seen = window if b == 1 else window & (kc >= first)
        far = jnp.where(seen, dist, jnp.inf)
        rows = slice(b * KEYS, (b + 1) * KEYS)
        for p in range(HEADS // 2):
            lanes = slice(p * 2 * HEAD_SIZE, (p + 1) * 2 * HEAD_SIZE)
            score = jnp.dot(q_ref[rows, lanes], kk[...], preferred_element_type=F32)
            probs = []
            for h in range(2):
                j = 2 * p + h
                one = score[:, h * 2 * KEYS : (h + 1) * 2 * KEYS] * HEAD_SIZE**-0.5
                one = one - far * (tier * 2.0 ** (-(j + 1) / 2))
                sink = jnp.broadcast_to(sink_ref[0:1, j : j + 1], (KEYS, 1))
                peak = jnp.maximum(jnp.max(one, axis=-1, keepdims=True), sink)
                e = jnp.exp(one - peak)
                denom = jnp.sum(e, axis=-1, keepdims=True) + jnp.exp(sink - peak)
                probs.append((e * (1.0 / denom)).astype(BF16))
            both = jnp.concatenate(probs, axis=1)
            o = lax.dot_general(
                both, vv[...], (((1,), (1,)), ((), ())), preferred_element_type=F32
            )
            att[rows, lanes] = o.astype(BF16)

    def piece(k):
        cols = slice(k * W, (k + 1) * W)
        return pltpu.make_async_remote_copy(
            src_ref=pj.at[1 - tp, :, cols],
            dst_ref=pjr.at[:, cols],
            send_sem=jsend.at[k],
            recv_sem=jrecv.at[k],
            device_id=partner,
            device_id_type=MESH,
        )

    def project(b):
        rows = slice(b * KEYS, (b + 1) * KEYS)
        for k in range(Q):
            cols = slice(k * W, (k + 1) * W)
            pj[b, :, cols] = jnp.dot(att[rows], wo[:, cols], preferred_element_type=F32)
            if b == 0:
                piece(k).start()

    def spots(g):
        return [
            ((z + dz) % 4) * 16 + ((y + dy) % 4) * 4 + (x + dx) % 4 for dx, dy, dz in CHUNKS[g]
        ]

    def sources(g):
        return [
            ((z + 4 - dz) % 4) * 16 + ((y + 4 - dy) % 4) * 4 + (x + 4 - dx) % 4
            for dx, dy, dz in CHUNKS[g]
        ]

    r0, r1 = routes_ref[0:1, :], routes_ref[1:2, :]
    ri, ci = fiota((ROWS, ROWS), 0), fiota((ROWS, ROWS), 1)
    eye = jnp.where(ri == ci, 1.0, 0.0)
    br = fiota((BLK, ROWS), 0)
    bq = fdiv(br, CAP)
    bs = br - bq * CAP

    def select(g):
        upper = jnp.where(ri < ci, 1.0, 0.0).astype(BF16)
        row = lax.broadcasted_iota(jnp.int32, (PER, ROWS), 0)
        e = jnp.zeros((PER, ROWS), jnp.int32)
        for i, spot in enumerate(spots(g)):
            e = jnp.where(row == i, spot, e)
        cnt = jnp.where((e == r0) | (e == r1), 1.0, 0.0)
        rank = jnp.dot(cnt.astype(BF16), upper, preferred_element_type=F32)
        code = jnp.where(cnt > 0.0, rank, -1.0)
        code = jnp.broadcast_to(code[:, None, :], (PER, BLK, ROWS))
        for k in range(Q):
            want = jnp.where(bq == k, bs, -2.0)
            hit = jnp.where(code == want[None], 1.0, 0.0).reshape(PER * BLK, ROWS)
            onehot[g, :, k * ROWS : (k + 1) * ROWS] = hit.astype(BF16)

    def column(v):
        return jnp.sum(eye * v.astype(F32), axis=1, keepdims=True)

    def weigh(g, c0, c1, w0, w1):
        lower = jnp.where(ci < ri, 1.0, 0.0).astype(BF16)
        lane = fiota((8, PER * BLK), 1)
        i = fdiv(lane, BLK)
        quarter = fdiv(lane - i * BLK, CAP)
        slot = (lane - i * BLK - quarter * CAP)[0:1]
        e = jnp.zeros((8, PER * BLK), F32)
        for n, spot in enumerate(spots(g)):
            e = jnp.where(i == n, spot.astype(F32), e)
        e = e[0:1]
        quarter = quarter[0:1]
        is0, is1 = e == c0, e == c1
        cnt = jnp.where(is0 | is1, 1.0, 0.0)
        rank = jnp.dot(lower, cnt.astype(BF16), preferred_element_type=F32)
        wt = jnp.where(is0, w0, 0.0) + jnp.where(is1, w1, 0.0)
        wt = jnp.where(rank == slot, wt, 0.0)
        hi = wt.astype(BF16).astype(F32)
        lo = wt - hi
        for k in range(Q):
            rows = slice(k * ROWS, (k + 1) * ROWS)
            comb_hi[g, rows] = jnp.where(quarter == k, hi, 0.0).astype(BF16)
            comb_lo[g, rows] = jnp.where(quarter == k, lo, 0.0).astype(BF16)

    def lo_of(g):
        return 1 if g == 0 else 0

    def exchange(g, src, dst, ssem, rsem, peers):
        for i in range(lo_of(g), PER):
            pltpu.make_async_remote_copy(
                src_ref=src.at[g * PER + i],
                dst_ref=dst.at[g * PER + i],
                send_sem=ssem.at[g],
                recv_sem=rsem.at[g],
                device_id=(peers[i], tp),
                device_id_type=MESH,
            ).start()

    def whole(g, src, dst, ssem, rsem):
        rows = pl.ds(g * PER + lo_of(g), PER - lo_of(g))
        return pltpu.make_async_remote_copy(
            src_ref=src.at[rows],
            dst_ref=dst.at[rows],
            send_sem=ssem.at[g],
            recv_sem=rsem.at[g],
            device_id=partner,
            device_id_type=MESH,
        )

    def forward(g):
        rows = pl.ds(g * PER, PER)
        return pltpu.make_async_remote_copy(
            src_ref=mine.at[rows],
            dst_ref=other.at[rows],
            send_sem=fsend.at[g],
            recv_sem=frecv.at[g],
            device_id=partner,
            device_id_type=MESH,
        )

    def swap(g, h):
        return pltpu.make_async_remote_copy(
            src_ref=po.at[g, h],
            dst_ref=pr.at[g, h],
            send_sem=psend.at[g, h],
            recv_sem=precv.at[g, h],
            device_id=partner,
            device_id_type=MESH,
        )

    def dispatch(g):
        rows = jnp.dot(onehot[g], nrm[...], preferred_element_type=F32).astype(BF16)
        rows = rows.reshape(PER, BLK, W)
        sbuf[pl.ds(g * PER, PER)] = rows
        if g == 0:
            mine[0] = rows[0]

    def send(g):
        exchange(g, sbuf, mine, dsend, drecv, spots(g))

    def permutation(inverse):
        pi, pj_ = fiota((GB * BLK, GB * BLK), 0), fiota((GB * BLK, GB * BLK), 1)
        a, b = (pj_, pi) if inverse else (pi, pj_)
        iq = fdiv(a, GR)
        ib = fdiv(a - iq * GR, CAP)
        ist = a - iq * GR - ib * CAP
        return jnp.where(ib * BLK + iq * CAP + ist == b, 1.0, 0.0).astype(BF16)

    def spread(g):
        unpack = permutation(False)
        for h in range(4):
            src = mine if h < 2 else other
            blocks = src[pl.ds(g * PER + (h % 2) * GB, GB)].reshape(GB * BLK, W)
            rows = jnp.dot(unpack, blocks, preferred_element_type=F32).astype(BF16)
            for q in range(Q):
                xbuf[h * GR : (h + 1) * GR, q * W : (q + 1) * W] = rows[q * GR : (q + 1) * GR]

    def gate_up(tiles):
        for k in tiles:
            cols = slice(k * 256, (k + 1) * 256)
            a = jnp.dot(xbuf[...], wg[:, cols], preferred_element_type=F32)
            b = jnp.dot(xbuf[...], wu[:, cols], preferred_element_type=F32)
            hid[:, cols] = (a / (1.0 + jnp.exp(-a)) * b).astype(BF16)

    def down(g):
        for k in range(Q):
            cols = slice(k * W, (k + 1) * W)
            a = jnp.dot(hid[...], wd[:, cols], preferred_element_type=F32).astype(BF16)
            pm[g % 2, :, cols] = a[: 2 * GR]
            po[g, k // 2, :, (k % 2) * W : (k % 2 + 1) * W] = a[2 * GR :]
            if k % 2 == 1:
                swap(g, k // 2).start()

    def give_back(g):
        pack = permutation(True)
        swap(g, 0).wait_recv()
        swap(g, 1).wait_recv()
        for h in range(2):
            rows = slice(h * GR, (h + 1) * GR)
            stack = []
            for k in range(Q):
                a = pm[g % 2, rows, k * W : (k + 1) * W].astype(F32)
                b = pr[g, k // 2, rows, (k % 2) * W : (k % 2 + 1) * W].astype(F32)
                stack.append((a + b).astype(BF16))
            packed = jnp.dot(pack, jnp.concatenate(stack, axis=0), preferred_element_type=F32)
            packed = packed.astype(BF16).reshape(GB, BLK, W)
            ysend[pl.ds(g * PER + h * GB, GB)] = packed
            if g == 0 and h == 0:
                zbuf[0] = packed[0]
        exchange(g, ysend, zbuf, rsend, rrecv, sources(g))

    def combine(g):
        whole(g, ysend, zbuf, rsend, rrecv).wait_recv()
        back = zbuf[pl.ds(g * PER, PER)].reshape(PER * BLK, W)
        both = jnp.dot(comb_hi[g], back, preferred_element_type=F32) + jnp.dot(
            comb_lo[g], back, preferred_element_type=F32
        )
        if g + 1 < CH:
            acc[...] += both
        else:
            total = (acc[...] + both).astype(BF16)
            for k in range(Q):
                out_ref[:, k * W : (k + 1) * W] = total[k * ROWS : (k + 1) * ROWS]

    attend(1)
    for c in ocopies:
        c.wait()
    for c in wcopies:
        c.start()
    project(1)
    for g in range(CH):
        select(g)
    pl.semaphore_wait(barrier, 64)
    whole_halo = pltpu.make_async_remote_copy(
        src_ref=halo,
        dst_ref=halo,
        send_sem=hsend,
        recv_sem=hrecv,
        device_id=((sp + 1) % 64, tp),
        device_id_type=MESH,
    )

    @pl.when(sp < 63)
    def _():
        for n, ref in enumerate((kt_ref, vt_ref)):
            pltpu.make_async_remote_copy(
                src_ref=ref.at[:, KEYS:],
                dst_ref=halo.at[n],
                send_sem=hsend,
                recv_sem=hrecv,
                device_id=((sp + 1) % 64, tp),
                device_id_type=MESH,
            ).start()

    wcol = [column(v) for v in (r0, r1, rw_ref[0:1, :], rw_ref[1:2, :])]
    for g in range(CH):
        weigh(g, *wcol)

    @pl.when(sp == 0)
    def _():
        halo[...] = jnp.zeros_like(halo)

    @pl.when(sp > 0)
    def _():
        whole_halo.wait_recv()

    attend(0)
    project(0)

    total = jnp.zeros((ROWS, 1), F32)
    for k in range(Q):
        piece(k).wait_recv()
        cols = slice(k * W, (k + 1) * W)
        m = res[:, cols].astype(F32) + (pj[tp, :, cols] + pjr[:, cols])
        acc[k * ROWS : (k + 1) * ROWS, :] = m
        total = total + jnp.sum(m * m, axis=-1, keepdims=True)
    scale = lax.rsqrt(total * (1.0 / D) + 1e-05)
    for k in range(Q):
        rows = slice(k * ROWS, (k + 1) * ROWS)
        gain = gain_ref[:, k * W : (k + 1) * W]
        nrm[rows] = (acc[rows] * scale * gain).astype(BF16)
    dispatch(0)
    send(0)
    dispatch(1)
    whole(0, sbuf, mine, dsend, drecv).wait_send()
    send(1)
    dispatch(2)
    dispatch(3)
    whole(0, sbuf, mine, dsend, drecv).wait_recv()
    forward(0).start()
    for c in wcopies:
        c.wait()
    for g in range(CH):
        forward(g).wait_recv()
        spread(g)
        gate_up(range(3))
        if g == 0:
            send(2)
        if g > 0:
            give_back(g - 1)
        gate_up(range(3, FFH // 256))
        if g == 0:
            send(3)
        if g + 1 < CH:
            whole(g + 1, sbuf, mine, dsend, drecv).wait_recv()
            forward(g + 1).start()
        down(g)
    give_back(CH - 1)
    for g in range(CH):
        combine(g)

    @pl.when(sp < 63)
    def _():
        whole_halo.wait_send()

    for k in range(Q):
        piece(k).wait_send()
    for g in range(CH):
        if g > 0:
            whole(g, sbuf, mine, dsend, drecv).wait_send()
        forward(g).wait_send()
        swap(g, 0).wait_send()
        swap(g, 1).wait_send()
        whole(g, ysend, zbuf, rsend, rrecv).wait_send()


def on_device(
    query_rows,
    key_rows,
    value_head_rows,
    sink_logit_head,
    out_weight,
    residual,
    norm_gain,
    routes,
    route_weights,
    gate_proj,
    up_proj,
    down_proj,
):
    vm = pl.BlockSpec(memory_space=pltpu.VMEM)
    hbm = pl.BlockSpec(memory_space=pl.ANY)
    sem = pltpu.SemaphoreType.DMA
    blocks = pltpu.VMEM((CH * PER, BLK, W), BF16)
    return pl.pallas_call(
        layer_kernel,
        out_shape=jax.ShapeDtypeStruct((ROWS, D), BF16),
        in_specs=[vm] * 7 + [hbm] * 5,
        out_specs=vm,
        scratch_shapes=[
            pltpu.VMEM((HEADS * HEAD_SIZE, D), BF16),
            pltpu.VMEM((ROWS, D), BF16),
            pltpu.VMEM((D, FFH), BF16),
            pltpu.VMEM((D, FFH), BF16),
            pltpu.VMEM((FFH, D), BF16),
            pltpu.VMEM((2, HEAD_SIZE, KEYS), BF16),
            pltpu.VMEM((2 * HEAD_SIZE, 4 * KEYS), BF16),
            pltpu.VMEM((2 * HEAD_SIZE, 4 * KEYS), BF16),
            pltpu.VMEM((2 * KEYS, HEADS * HEAD_SIZE), BF16),
            pltpu.VMEM((2, ROWS, D), F32),
            pltpu.VMEM((ROWS, D), F32),
            pltpu.VMEM((Q * ROWS, W), BF16),
            pltpu.VMEM((CH, PER * BLK, Q * ROWS), BF16),
            pltpu.VMEM((CH, Q * ROWS, PER * BLK), BF16),
            pltpu.VMEM((CH, Q * ROWS, PER * BLK), BF16),
            blocks,
            blocks,
            blocks,
            pltpu.VMEM((4 * GR, D), BF16),
            pltpu.VMEM((4 * GR, FFH), BF16),
            pltpu.VMEM((2, 2 * GR, D), BF16),
            pltpu.VMEM((CH, 2, 2 * GR, D // 2), BF16),
            pltpu.VMEM((CH, 2, 2 * GR, D // 2), BF16),
            blocks,
            blocks,
            pltpu.VMEM((Q * ROWS, W), F32),
            sem((2,)),
            sem((3, 4)),
            sem,
            sem,
            sem((Q,)),
            sem((Q,)),
            sem((CH,)),
            sem((CH,)),
            sem((CH,)),
            sem((CH,)),
            sem((CH, 2)),
            sem((CH, 2)),
            sem((CH,)),
            sem((CH,)),
        ],
        compiler_params=pltpu.CompilerParams(
            collective_id=0, has_side_effects=True, vmem_limit_bytes=60 * 1024 * 1024
        ),
        name="layer",
    )(
        query_rows,
        key_rows.T,
        value_head_rows.T,
        sink_logit_head.reshape(1, HEADS),
        norm_gain.reshape(1, D),
        routes.T,
        route_weights.T,
        out_weight,
        residual,
        gate_proj,
        up_proj,
        down_proj,
    )


def solution(mesh):
    placed = (
        P("sp", "tp"),
        P("sp", "tp"),
        P("sp", "tp"),
        P("tp"),
        P("tp", None),
        P(("sp", "tp"), None),
        P(),
        P(("sp", "tp"), None),
        P(("sp", "tp"), None),
        P("sp", None, "tp"),
        P("sp", None, "tp"),
        P("sp", "tp", None),
    )
    return jax.shard_map(
        on_device, mesh=mesh, in_specs=placed, out_specs=P(("sp", "tp"), None), check_vma=False
    )
```

```python
import jax
import jax.numpy as jnp
from jax import lax
from jax.experimental import pallas as pl
from jax.experimental.pallas import tpu as pltpu
from jax.sharding import PartitionSpec as P

MESH = pl.DeviceIdType.MESH
F32 = jnp.float32
BF16 = jnp.bfloat16

HEADS = 8
HEAD_SIZE = 64
KEYS = 128
ROWS = 128
D = 2048
FFH = 1792
CAP = 6
Q = 4
W = D // Q
BLK = Q * CAP
CH = 4
PER = 16
GB = 8
GR = GB * CAP


def offset_chunks():
    def hops(o):
        return sum(min(v, 4 - v) for v in o)

    def opposite(o):
        return tuple((4 - v) % 4 for v in o)

    every = [(a, b, c) for a in range(4) for b in range(4) for c in range(4)]
    by = {h: [o for o in every if hops(o) == h] for h in range(7)}
    axial = [o for o in by[2] if 2 in o]
    same = [o for o in by[2] if 2 not in o and len(set(v for v in o if v)) == 1]
    mixed = [o for o in by[2] if 2 not in o and o not in same]
    corners = [o for o in by[3] if 2 not in o]
    sides = [o for o in by[3] if 2 in o]
    first = by[0] + by[1] + axial + same
    last = corners + sides[:1] + [opposite(sides[0])] + mixed
    rest = [o for o in by[6] + by[5] + by[4] + by[3] if o not in last]
    rest.sort(key=hops, reverse=True)
    return [first, rest[:PER], rest[PER:], last]


CHUNKS = offset_chunks()


def fiota(shape, dim):
    return lax.broadcasted_iota(jnp.int32, shape, dim).astype(F32)


def fdiv(v, n):
    return jnp.floor((v + 0.5) * (1.0 / n))


def layer_kernel(
    q_ref,
    kt_ref,
    vt_ref,
    sink_ref,
    gain_ref,
    routes_ref,
    rw_ref,
    wo_hbm,
    res_hbm,
    wg_hbm,
    wu_hbm,
    wd_hbm,
    out_ref,
    wo,
    res,
    wg,
    wu,
    wd,
    halo,
    kk,
    vv,
    att,
    pj,
    pjr,
    nrm,
    onehot,
    comb_hi,
    comb_lo,
    sbuf,
    mine,
    other,
    xbuf,
    hid,
    pm,
    po,
    pr,
    ysend,
    zbuf,
    acc,
    osem,
    wsem,
    hsend,
    hrecv,
    jsend,
    jrecv,
    dsend,
    drecv,
    fsend,
    frecv,
    psend,
    precv,
    rsend,
    rrecv,
):
    sp = lax.axis_index("sp")
    tp = lax.axis_index("tp")
    x, y, z = sp % 4, (sp // 4) % 4, sp // 16
    partner = (sp, 1 - tp)

    barrier = pltpu.get_barrier_semaphore()

    def greet(i, _):
        pl.semaphore_signal(barrier, inc=1, device_id=((sp + i) % 64, tp), device_id_type=MESH)
        return 0

    lax.fori_loop(1, 64, greet, 0)
    pl.semaphore_signal(barrier, inc=1, device_id=partner, device_id_type=MESH)

    ocopies = [
        pltpu.make_async_copy(wo_hbm, wo, osem.at[0]),
        pltpu.make_async_copy(res_hbm, res, osem.at[1]),
    ]
    for c in ocopies:
        c.start()
    wcopies = []
    for k, (src, dst) in enumerate(((wg_hbm, wg), (wu_hbm, wu), (wd_hbm, wd))):
        part = src.shape[1] // 4
        for j in range(4):
            rows = pl.ds(j * part, part)
            wcopies.append(pltpu.make_async_copy(src.at[0, rows], dst.at[rows], wsem.at[k, j]))

    qi, kc = fiota((KEYS, 2 * KEYS), 0), fiota((KEYS, 2 * KEYS), 1)
    dist = qi + KEYS - kc
    window = (dist >= 0.0) & (dist < KEYS)
    tier = jnp.where(tp == 0, 1.0, 2.0 ** (-HEADS / 2)).astype(F32)
    first = jnp.where(sp == 0, float(KEYS), 0.0).astype(F32)
    kk[...] = jnp.zeros_like(kk)
    vv[...] = jnp.zeros_like(vv)

    def attend(b):
        for ref, own, n in ((kk, kt_ref, 0), (vv, vt_ref, 1)):
            for h in range(2):
                rows = slice(h * HEAD_SIZE, (h + 1) * HEAD_SIZE)
                lane = h * 2 * KEYS
                if b == 1:
                    ref[rows, lane : lane + 2 * KEYS] = own[...]
                else:
                    ref[rows, lane : lane + KEYS] = halo[n]
                    ref[rows, lane + KEYS : lane + 2 * KEYS] = own[:, :KEYS]
        seen = window if b == 1 else window & (kc >= first)
        far = jnp.where(seen, dist, jnp.inf)
        rows = slice(b * KEYS, (b + 1) * KEYS)
        for p in range(HEADS // 2):
            lanes = slice(p * 2 * HEAD_SIZE, (p + 1) * 2 * HEAD_SIZE)
            score = jnp.dot(q_ref[rows, lanes], kk[...], preferred_element_type=F32)
            probs = []
            for h in range(2):
                j = 2 * p + h
                one = score[:, h * 2 * KEYS : (h + 1) * 2 * KEYS] * HEAD_SIZE**-0.5
                one = one - far * (tier * 2.0 ** (-(j + 1) / 2))
                sink = jnp.broadcast_to(sink_ref[0:1, j : j + 1], (KEYS, 1))
                peak = jnp.maximum(jnp.max(one, axis=-1, keepdims=True), sink)
                e = jnp.exp(one - peak)
                denom = jnp.sum(e, axis=-1, keepdims=True) + jnp.exp(sink - peak)
                probs.append((e * (1.0 / denom)).astype(BF16))
            both = jnp.concatenate(probs, axis=1)
            o = lax.dot_general(
                both, vv[...], (((1,), (1,)), ((), ())), preferred_element_type=F32
            )
            att[rows, lanes] = o.astype(BF16)

    def piece(k):
        cols = slice(k * W, (k + 1) * W)
        return pltpu.make_async_remote_copy(
            src_ref=pj.at[1 - tp, :, cols],
            dst_ref=pjr.at[:, cols],
            send_sem=jsend.at[k],
            recv_sem=jrecv.at[k],
            device_id=partner,
            device_id_type=MESH,
        )

    def project(b):
        rows = slice(b * KEYS, (b + 1) * KEYS)
        for k in range(Q):
            cols = slice(k * W, (k + 1) * W)
            pj[b, :, cols] = jnp.dot(att[rows], wo[:, cols], preferred_element_type=F32)
            if b == 0:
                piece(k).start()

    def spots(g):
        return [
            ((z + dz) % 4) * 16 + ((y + dy) % 4) * 4 + (x + dx) % 4 for dx, dy, dz in CHUNKS[g]
        ]

    def sources(g):
        return [
            ((z + 4 - dz) % 4) * 16 + ((y + 4 - dy) % 4) * 4 + (x + 4 - dx) % 4
            for dx, dy, dz in CHUNKS[g]
        ]

    r0, r1 = routes_ref[0:1, :], routes_ref[1:2, :]
    ri, ci = fiota((ROWS, ROWS), 0), fiota((ROWS, ROWS), 1)
    eye = jnp.where(ri == ci, 1.0, 0.0)
    br = fiota((BLK, ROWS), 0)
    bq = fdiv(br, CAP)
    bs = br - bq * CAP

    def select(g):
        upper = jnp.where(ri < ci, 1.0, 0.0).astype(BF16)
        row = lax.broadcasted_iota(jnp.int32, (PER, ROWS), 0)
        e = jnp.zeros((PER, ROWS), jnp.int32)
        for i, spot in enumerate(spots(g)):
            e = jnp.where(row == i, spot, e)
        cnt = jnp.where((e == r0) | (e == r1), 1.0, 0.0)
        rank = jnp.dot(cnt.astype(BF16), upper, preferred_element_type=F32)
        code = jnp.where(cnt > 0.0, rank, -1.0)
        code = jnp.broadcast_to(code[:, None, :], (PER, BLK, ROWS))
        for k in range(Q):
            want = jnp.where(bq == k, bs, -2.0)
            hit = jnp.where(code == want[None], 1.0, 0.0).reshape(PER * BLK, ROWS)
            onehot[g, :, k * ROWS : (k + 1) * ROWS] = hit.astype(BF16)

    def column(v):
        return jnp.sum(eye * v.astype(F32), axis=1, keepdims=True)

    def weigh(g, c0, c1, w0, w1):
        lower = jnp.where(ci < ri, 1.0, 0.0).astype(BF16)
        lane = fiota((8, PER * BLK), 1)
        i = fdiv(lane, BLK)
        quarter = fdiv(lane - i * BLK, CAP)
        slot = (lane - i * BLK - quarter * CAP)[0:1]
        e = jnp.zeros((8, PER * BLK), F32)
        for n, spot in enumerate(spots(g)):
            e = jnp.where(i == n, spot.astype(F32), e)
        e = e[0:1]
        quarter = quarter[0:1]
        is0, is1 = e == c0, e == c1
        cnt = jnp.where(is0 | is1, 1.0, 0.0)
        rank = jnp.dot(lower, cnt.astype(BF16), preferred_element_type=F32)
        wt = jnp.where(is0, w0, 0.0) + jnp.where(is1, w1, 0.0)
        wt = jnp.where(rank == slot, wt, 0.0)
        hi = wt.astype(BF16).astype(F32)
        lo = wt - hi
        for k in range(Q):
            rows = slice(k * ROWS, (k + 1) * ROWS)
            comb_hi[g, rows] = jnp.where(quarter == k, hi, 0.0).astype(BF16)
            comb_lo[g, rows] = jnp.where(quarter == k, lo, 0.0).astype(BF16)

    def lo_of(g):
        return 1 if g == 0 else 0

    def exchange(g, src, dst, ssem, rsem, peers):
        for i in range(lo_of(g), PER):
            pltpu.make_async_remote_copy(
                src_ref=src.at[g * PER + i],
                dst_ref=dst.at[g * PER + i],
                send_sem=ssem.at[g],
                recv_sem=rsem.at[g],
                device_id=(peers[i], tp),
                device_id_type=MESH,
            ).start()

    def whole(g, src, dst, ssem, rsem):
        rows = pl.ds(g * PER + lo_of(g), PER - lo_of(g))
        return pltpu.make_async_remote_copy(
            src_ref=src.at[rows],
            dst_ref=dst.at[rows],
            send_sem=ssem.at[g],
            recv_sem=rsem.at[g],
            device_id=partner,
            device_id_type=MESH,
        )

    def forward(g):
        rows = pl.ds(g * PER, PER)
        return pltpu.make_async_remote_copy(
            src_ref=mine.at[rows],
            dst_ref=other.at[rows],
            send_sem=fsend.at[g],
            recv_sem=frecv.at[g],
            device_id=partner,
            device_id_type=MESH,
        )

    def swap(g, h):
        return pltpu.make_async_remote_copy(
            src_ref=po.at[g, h],
            dst_ref=pr.at[g, h],
            send_sem=psend.at[g, h],
            recv_sem=precv.at[g, h],
            device_id=partner,
            device_id_type=MESH,
        )

    def dispatch(g):
        rows = jnp.dot(onehot[g], nrm[...], preferred_element_type=F32).astype(BF16)
        rows = rows.reshape(PER, BLK, W)
        sbuf[pl.ds(g * PER, PER)] = rows
        if g == 0:
            mine[0] = rows[0]

    def send(g):
        exchange(g, sbuf, mine, dsend, drecv, spots(g))

    def permutation(inverse):
        pi, pj_ = fiota((GB * BLK, GB * BLK), 0), fiota((GB * BLK, GB * BLK), 1)
        a, b = (pj_, pi) if inverse else (pi, pj_)
        iq = fdiv(a, GR)
        ib = fdiv(a - iq * GR, CAP)
        ist = a - iq * GR - ib * CAP
        return jnp.where(ib * BLK + iq * CAP + ist == b, 1.0, 0.0).astype(BF16)

    def spread(g):
        unpack = permutation(False)
        for h in range(4):
            src = mine if h < 2 else other
            blocks = src[pl.ds(g * PER + (h % 2) * GB, GB)].reshape(GB * BLK, W)
            rows = jnp.dot(unpack, blocks, preferred_element_type=F32).astype(BF16)
            for q in range(Q):
                xbuf[h * GR : (h + 1) * GR, q * W : (q + 1) * W] = rows[q * GR : (q + 1) * GR]

    def gate_up(tiles):
        for k in tiles:
            cols = slice(k * 256, (k + 1) * 256)
            a = jnp.dot(xbuf[...], wg[:, cols], preferred_element_type=F32)
            b = jnp.dot(xbuf[...], wu[:, cols], preferred_element_type=F32)
            hid[:, cols] = (a / (1.0 + jnp.exp(-a)) * b).astype(BF16)

    def down(g):
        for k in range(Q):
            cols = slice(k * W, (k + 1) * W)
            a = jnp.dot(hid[...], wd[:, cols], preferred_element_type=F32).astype(BF16)
            pm[g % 2, :, cols] = a[: 2 * GR]
            po[g, k // 2, :, (k % 2) * W : (k % 2 + 1) * W] = a[2 * GR :]
            if k % 2 == 1:
                swap(g, k // 2).start()

    def give_back(g):
        pack = permutation(True)
        swap(g, 0).wait_recv()
        swap(g, 1).wait_recv()
        for h in range(2):
            rows = slice(h * GR, (h + 1) * GR)
            stack = []
            for k in range(Q):
                a = pm[g % 2, rows, k * W : (k + 1) * W].astype(F32)
                b = pr[g, k // 2, rows, (k % 2) * W : (k % 2 + 1) * W].astype(F32)
                stack.append((a + b).astype(BF16))
            packed = jnp.dot(pack, jnp.concatenate(stack, axis=0), preferred_element_type=F32)
            packed = packed.astype(BF16).reshape(GB, BLK, W)
            ysend[pl.ds(g * PER + h * GB, GB)] = packed
            if g == 0 and h == 0:
                zbuf[0] = packed[0]
        exchange(g, ysend, zbuf, rsend, rrecv, sources(g))

    def combine(g):
        whole(g, ysend, zbuf, rsend, rrecv).wait_recv()
        back = zbuf[pl.ds(g * PER, PER)].reshape(PER * BLK, W)
        both = jnp.dot(comb_hi[g], back, preferred_element_type=F32) + jnp.dot(
            comb_lo[g], back, preferred_element_type=F32
        )
        if g + 1 < CH:
            acc[...] += both
        else:
            total = (acc[...] + both).astype(BF16)
            for k in range(Q):
                out_ref[:, k * W : (k + 1) * W] = total[k * ROWS : (k + 1) * ROWS]

    attend(1)
    for c in ocopies:
        c.wait()
    for c in wcopies:
        c.start()
    project(1)
    for g in range(CH):
        select(g)
    pl.semaphore_wait(barrier, 64)
    whole_halo = pltpu.make_async_remote_copy(
        src_ref=halo,
        dst_ref=halo,
        send_sem=hsend,
        recv_sem=hrecv,
        device_id=((sp + 1) % 64, tp),
        device_id_type=MESH,
    )

    @pl.when(sp < 63)
    def _():
        for n, ref in enumerate((kt_ref, vt_ref)):
            pltpu.make_async_remote_copy(
                src_ref=ref.at[:, KEYS:],
                dst_ref=halo.at[n],
                send_sem=hsend,
                recv_sem=hrecv,
                device_id=((sp + 1) % 64, tp),
                device_id_type=MESH,
            ).start()

    wcol = [column(v) for v in (r0, r1, rw_ref[0:1, :], rw_ref[1:2, :])]
    for g in range(CH):
        weigh(g, *wcol)

    @pl.when(sp == 0)
    def _():
        halo[...] = jnp.zeros_like(halo)

    @pl.when(sp > 0)
    def _():
        whole_halo.wait_recv()

    attend(0)
    project(0)

    total = jnp.zeros((ROWS, 1), F32)
    for k in range(Q):
        piece(k).wait_recv()
        cols = slice(k * W, (k + 1) * W)
        m = res[:, cols].astype(F32) + (pj[tp, :, cols] + pjr[:, cols])
        acc[k * ROWS : (k + 1) * ROWS, :] = m
        total = total + jnp.sum(m * m, axis=-1, keepdims=True)
    scale = lax.rsqrt(total * (1.0 / D) + 1e-05)
    for k in range(Q):
        rows = slice(k * ROWS, (k + 1) * ROWS)
        gain = gain_ref[:, k * W : (k + 1) * W]
        nrm[rows] = (acc[rows] * scale * gain).astype(BF16)
    dispatch(0)
    send(0)
    dispatch(1)
    whole(0, sbuf, mine, dsend, drecv).wait_send()
    send(1)
    dispatch(2)
    dispatch(3)
    whole(0, sbuf, mine, dsend, drecv).wait_recv()
    forward(0).start()
    send(2)
    for c in wcopies:
        c.wait()
    for g in range(CH):
        forward(g).wait_recv()
        spread(g)
        gate_up(range(2))
        if g == 0:
            send(3)
        if g > 0:
            give_back(g - 1)
        gate_up(range(2, FFH // 256))
        if g + 1 < CH:
            whole(g + 1, sbuf, mine, dsend, drecv).wait_recv()
            forward(g + 1).start()
        down(g)
    give_back(CH - 1)
    for g in range(CH):
        combine(g)

    @pl.when(sp < 63)
    def _():
        whole_halo.wait_send()

    for k in range(Q):
        piece(k).wait_send()
    for g in range(CH):
        if g > 0:
            whole(g, sbuf, mine, dsend, drecv).wait_send()
        forward(g).wait_send()
        swap(g, 0).wait_send()
        swap(g, 1).wait_send()
        whole(g, ysend, zbuf, rsend, rrecv).wait_send()


def on_device(
    query_rows,
    key_rows,
    value_head_rows,
    sink_logit_head,
    out_weight,
    residual,
    norm_gain,
    routes,
    route_weights,
    gate_proj,
    up_proj,
    down_proj,
):
    vm = pl.BlockSpec(memory_space=pltpu.VMEM)
    hbm = pl.BlockSpec(memory_space=pl.ANY)
    sem = pltpu.SemaphoreType.DMA
    blocks = pltpu.VMEM((CH * PER, BLK, W), BF16)
    return pl.pallas_call(
        layer_kernel,
        out_shape=jax.ShapeDtypeStruct((ROWS, D), BF16),
        in_specs=[vm] * 7 + [hbm] * 5,
        out_specs=vm,
        scratch_shapes=[
            pltpu.VMEM((HEADS * HEAD_SIZE, D), BF16),
            pltpu.VMEM((ROWS, D), BF16),
            pltpu.VMEM((D, FFH), BF16),
            pltpu.VMEM((D, FFH), BF16),
            pltpu.VMEM((FFH, D), BF16),
            pltpu.VMEM((2, HEAD_SIZE, KEYS), BF16),
            pltpu.VMEM((2 * HEAD_SIZE, 4 * KEYS), BF16),
            pltpu.VMEM((2 * HEAD_SIZE, 4 * KEYS), BF16),
            pltpu.VMEM((2 * KEYS, HEADS * HEAD_SIZE), BF16),
            pltpu.VMEM((2, ROWS, D), F32),
            pltpu.VMEM((ROWS, D), F32),
            pltpu.VMEM((Q * ROWS, W), BF16),
            pltpu.VMEM((CH, PER * BLK, Q * ROWS), BF16),
            pltpu.VMEM((CH, Q * ROWS, PER * BLK), BF16),
            pltpu.VMEM((CH, Q * ROWS, PER * BLK), BF16),
            blocks,
            blocks,
            blocks,
            pltpu.VMEM((4 * GR, D), BF16),
            pltpu.VMEM((4 * GR, FFH), BF16),
            pltpu.VMEM((2, 2 * GR, D), BF16),
            pltpu.VMEM((CH, 2, 2 * GR, D // 2), BF16),
            pltpu.VMEM((CH, 2, 2 * GR, D // 2), BF16),
            blocks,
            blocks,
            pltpu.VMEM((Q * ROWS, W), F32),
            sem((2,)),
            sem((3, 4)),
            sem,
            sem,
            sem((Q,)),
            sem((Q,)),
            sem((CH,)),
            sem((CH,)),
            sem((CH,)),
            sem((CH,)),
            sem((CH, 2)),
            sem((CH, 2)),
            sem((CH,)),
            sem((CH,)),
        ],
        compiler_params=pltpu.CompilerParams(
            collective_id=0, has_side_effects=True, vmem_limit_bytes=60 * 1024 * 1024
        ),
        name="layer",
    )(
        query_rows,
        key_rows.T,
        value_head_rows.T,
        sink_logit_head.reshape(1, HEADS),
        norm_gain.reshape(1, D),
        routes.T,
        route_weights.T,
        out_weight,
        residual,
        gate_proj,
        up_proj,
        down_proj,
    )


def solution(mesh):
    placed = (
        P("sp", "tp"),
        P("sp", "tp"),
        P("sp", "tp"),
        P("tp"),
        P("tp", None),
        P(("sp", "tp"), None),
        P(),
        P(("sp", "tp"), None),
        P(("sp", "tp"), None),
        P("sp", None, "tp"),
        P("sp", None, "tp"),
        P("sp", "tp", None),
    )
    return jax.shard_map(
        on_device, mesh=mesh, in_specs=placed, out_specs=P(("sp", "tp"), None), check_vma=False
    )
```
